32 devices in a mesh: kv: 8 (over z, x), tp: 4 (over y, core).
Axes of the slice: x: 2, y: 2, z: 4, core: 2. Of those that a mesh axis runs over, the one named last changes fastest.
Arguments:
- tokens: bfloat16 [64, 12, 4096], P(None, None, 'kv'), may hold values from -6 to 6
- parents: int32 [64, 12], P('kv'), may hold values from -1 to 10, as said below
- accepted: int32 [64], P('kv'), may hold values from 0 to 6
- state: float32 [64, 64, 64, 128], P('kv', 'tp'), may hold values from -4 to 4
- conv_x: bfloat16 [64, 3, 4096], P('kv', None, 'tp'), may hold values from -6 to 6
- conv_b: bfloat16 [64, 3, 2048], P('kv', None, 'tp'), may hold values from -6 to 6
- conv_c: bfloat16 [64, 3, 2048], P('kv', None, 'tp'), may hold values from -6 to 6
- path_x: bfloat16 [64, 6, 4096], P('kv', None, 'tp'), may hold values from -6 to 6
- path_b: bfloat16 [64, 6, 2048], P('kv', None, 'tp'), may hold values from -6 to 6
- path_c: bfloat16 [64, 6, 2048], P('kv', None, 'tp'), may hold values from -6 to 6
- path_dt: bfloat16 [64, 6, 64], P('kv', None, 'tp'), may hold values from -6 to 6
- gain_in: float32 [4096], replicated, may hold values from 0.1 to 1.9
- w_x: bfloat16 [4096, 4096], P('kv', 'tp'), may hold values from -0.09375 to 0.09375
- w_z: bfloat16 [4096, 4096], P('kv', 'tp'), may hold values from -0.09375 to 0.09375
- w_b: bfloat16 [4096, 2048], P('kv', 'tp'), may hold values from -0.09375 to 0.09375
- w_c: bfloat16 [4096, 2048], P('kv', 'tp'), may hold values from -0.09375 to 0.09375
- w_dt: bfloat16 [4096, 64], replicated, may hold values from -0.09375 to 0.09375
- dt_bias: float32 [64], P('tp'), may hold values from -2 to 1
- a_log: float32 [64], P('tp'), may hold values from -3 to 1.5
- d_skip: float32 [64], P('tp'), may hold values from 0.5 to 1.5
- conv_wx: bfloat16 [4, 4096], P(None, 'tp'), may hold values from -3 to 3
- conv_wb: bfloat16 [4, 2048], P(None, 'tp'), may hold values from -3 to 3
- conv_wc: bfloat16 [4, 2048], P(None, 'tp'), may hold values from -3 to 3
- gain_out: float32 [4096], P('tp'), may hold values from 0.1 to 1.9
- w_out: bfloat16 [4096, 4096], P('tp', 'kv'), may hold values from -0.09375 to 0.09375
Outputs:
- mixed: bfloat16 [64, 12, 4096], P('kv', None, 'tp')
- new_state: float32 [64, 64, 64, 128], P('kv', 'tp')
The draws below stay inside these ranges and needn't reach their ends.
Inputs may be any that keep to these rules, and one draw needn't show every extreme that they name: `parents`: each proposal's parent is -1 or an earlier proposal of the same sequence; the first proposal's parent is -1.
All inputs are finite; a program needn't handle non-finite values.
Results may differ from the reference program's by a relative error of at most 0.03.
Values may be sent and summed in bfloat16 or wider, within the bound.
A program may use at most 128 MiB of HBM per device.

```python
import jax
import jax.numpy as jnp
from jax import lax

D = 4096
G = 16
HPG = 4
H = 64
HD = 64
N = 128
INNER = 4096
CONV = 4
Q = 12
P_SIZE = 6
SEQS = 64
N_TP = 4


def draw_parents(key, part):
    jumps = jax.random.randint(key, (SEQS, Q), 0, 3)
    places = jnp.arange(Q, dtype=jnp.int32)[None, :]
    return jnp.maximum(places - 1 - jumps, -1).astype(jnp.int32)


def touch_ends(array, key, low, largest):
    longest = array.shape.index(max(array.shape))
    spots = []
    for shift in (0, 1):
        where = [jax.random.randint(jax.random.fold_in(key, axis), (), 0, length) for axis, length in enumerate(array.shape)]
        where[longest] = (where[longest] + shift) % array.shape[longest]
        spots.append(tuple(where))
    return array.at[spots[0]].set(low).at[spots[1]].set(largest)


def raised(values, stream_key, source, target, shards_of, factor):
    def block_of(position):
        return (jnp.arange(values.shape[position]) // (values.shape[position] // shards_of)).reshape((-1,) + (1,) * (values.ndim - 1 - position))

    near = jax.random.permutation(stream_key, shards_of)[block_of(target)]
    second = (block_of(target) + shards_of // 2) % shards_of
    return jnp.where((block_of(source) == near) | (block_of(source) == second), factor * values, values)


def block_scale(key, extent, split, smallest, high):
    gain = 1.0
    for dim, blocks in split:
        steps = jax.random.uniform(jax.random.fold_in(jax.random.fold_in(key, 6), dim), (blocks,), jnp.float32, smallest / len(split), high / len(split))
        gain = gain * jnp.repeat(jnp.exp(steps), extent[dim] // blocks).reshape((-1,) + (1,) * (len(extent) - 1 - dim))
    return gain


def noise(rng, dims, spread, bound, shards=(), kind=jnp.bfloat16):
    array = jax.random.normal(rng, dims, jnp.float32) * spread
    if len(shards) > 0:
        array = block_scale(rng, dims, shards, -0.22, 0.18) * array
    return jnp.clip(array, min=-bound, max=bound).astype(kind)


def heavy_noise(own_key, shape, deviation, reach, shards, heavy, kind=jnp.bfloat16):
    array = deviation * jax.random.normal(own_key, shape, jnp.float32)
    if shards:
        array = array * block_scale(own_key, shape, shards, -0.22, 0.18)
    return jnp.clip(raised(array, jax.random.fold_in(own_key, 3), *heavy), -reach, reach).astype(kind)


def setup_inputs(seed: int = 0) -> dict:
    key_list = jax.random.split(jax.random.key(seed), 26)
    tokens = heavy_noise(key_list[0], (SEQS, Q, D), 1.0, 6.0, ((2, 8),), (2, 0, 8, 2.0))
    parents = draw_parents(jax.random.fold_in(key_list[25], 71), 0)
    accepted = touch_ends(jax.random.randint(key_list[2], (SEQS,), 0, P_SIZE + 1), jax.random.fold_in(key_list[2], 1), 0, P_SIZE).astype(jnp.int32)
    state = noise(key_list[3], (SEQS, H, HD, N), 0.3, 4.0, ((0, 8), (1, 4)), jnp.float32)
    conv_x = noise(key_list[4], (SEQS, CONV - 1, INNER), 1.0, 6.0, ((0, 8), (2, 4)))
    conv_b = noise(key_list[5], (SEQS, CONV - 1, G * N), 1.0, 6.0, ((0, 8), (2, 4)))
    conv_c = noise(key_list[6], (SEQS, CONV - 1, G * N), 1.0, 6.0, ((0, 8), (2, 4)))
    path_x = noise(key_list[7], (SEQS, P_SIZE, INNER), 1.0, 6.0, ((0, 8), (2, 4)))
    path_b = noise(key_list[8], (SEQS, P_SIZE, G * N), 1.0, 6.0, ((0, 8), (2, 4)))
    path_c = noise(key_list[9], (SEQS, P_SIZE, G * N), 1.0, 6.0, ((0, 8), (2, 4)))
    path_dt = noise(key_list[10], (SEQS, P_SIZE, H), 1.0, 6.0, ((0, 8), (2, 4)))
    gain_in = jnp.clip(1.0 + 0.18 * jax.random.normal(key_list[11], (D,), jnp.float32), 0.1, 1.9)
    w_x = noise(key_list[12], (D, INNER), D ** -0.5, 0.09375, ((0, 8), (1, 4)))
    w_z = noise(key_list[13], (D, INNER), D ** -0.5, 0.09375, ((0, 8), (1, 4)))
    w_b = noise(key_list[14], (D, G * N), D ** -0.5, 0.09375, ((0, 8), (1, 4)))
    w_c = noise(key_list[15], (D, G * N), D ** -0.5, 0.09375, ((0, 8), (1, 4)))
    w_dt = noise(key_list[16], (D, H), D ** -0.5, 0.09375)
    dt_bias = jnp.clip(-2.0 + 3.0 * jax.random.uniform(key_list[17], (H,), jnp.float32) ** block_scale(key_list[17], (H,), ((0, 4),), -0.2, 0.2), -2.0, 1.0)
    a_log = jnp.clip(-3.0 + 4.5 * jax.random.uniform(key_list[18], (H,), jnp.float32) ** block_scale(key_list[18], (H,), ((0, 4),), -0.2, 0.2), -3.0, 1.5)
    d_skip = jnp.clip(0.5 + 1.0 * jax.random.uniform(key_list[19], (H,), jnp.float32) ** block_scale(key_list[19], (H,), ((0, 4),), -0.2, 0.2), 0.5, 1.5)
    conv_wx = noise(key_list[20], (CONV, INNER), 0.5, 3.0, ((1, 4),))
    conv_wb = noise(key_list[21], (CONV, G * N), 0.5, 3.0, ((1, 4),))
    conv_wc = noise(key_list[22], (CONV, G * N), 0.5, 3.0, ((1, 4),))
    gain_out = jnp.clip(1.0 + 0.18 * jax.random.normal(key_list[23], (INNER,), jnp.float32), 0.1, 1.9)
    w_out = noise(key_list[24], (INNER, D), INNER ** -0.5, 0.09375, ((0, 4), (1, 8)))
    return dict(tokens=tokens, parents=parents, accepted=accepted, state=state, conv_x=conv_x, conv_b=conv_b, conv_c=conv_c, path_x=path_x, path_b=path_b, path_c=path_c, path_dt=path_dt, gain_in=gain_in, w_x=w_x, w_z=w_z, w_b=w_b, w_c=w_c, w_dt=w_dt, dt_bias=dt_bias, a_log=a_log, d_skip=d_skip, conv_wx=conv_wx, conv_wb=conv_wb, conv_wc=conv_wc, gain_out=gain_out, w_out=w_out)


EPS = 1e-06
HIGH = lax.Precision.HIGHEST

def conv_window(history, taps, amount):
    values = history.astype(jnp.float32)
    weights = taps.astype(jnp.float32)
    summed = weights[0] * values[:, 0:amount, :]
    for distance in range(1, weights.shape[0]):
        summed = summed + weights[distance] * values[:, distance:distance + amount, :]
    return jax.nn.silu(summed)

def commit_rows(history, accepted, keep):
    picked = accepted[:, None].astype(jnp.int32) + jnp.arange(keep, dtype=jnp.int32)[None, :]
    select = (picked[:, :, None] == jnp.arange(history.shape[1], dtype=jnp.int32)[None, None, :]).astype(jnp.float32)
    return jnp.einsum('skl,slc->skc', select, history.astype(jnp.float32), precision=HIGH).astype(jnp.bfloat16)

def replay_state(state, history_x, history_b, path_dt, conv_wx, conv_wb, accepted, rate_bias, a_rate, per_group):
    seq_count, heads, head_dim, state_dim = state.shape
    path_len = path_dt.shape[1]
    path_xs = conv_window(history_x, conv_wx, path_len).reshape(seq_count, path_len, heads, head_dim)
    path_bs = conv_window(history_b, conv_wb, path_len).reshape(seq_count, path_len, heads // per_group, state_dim)
    path_bh = jnp.repeat(path_bs, per_group, axis=2)
    path_step = jax.nn.softplus(path_dt.astype(jnp.float32) + rate_bias)
    is_live = (jnp.arange(path_len, dtype=jnp.int32)[None, :] < accepted[:, None].astype(jnp.int32)).astype(jnp.float32)[:, :, None]
    log_decay = path_step * a_rate * is_live
    overall = lax.optimization_barrier(jnp.sum(log_decay, axis=1))
    tail_sum = overall[:, None, :] - jnp.cumsum(log_decay, axis=1)
    weights = is_live * jnp.exp(tail_sum) * path_step
    grown = jnp.einsum('sjh,sjhp,sjhn->shpn', weights, path_xs, path_bh, precision=HIGH)
    return jnp.exp(overall)[:, :, None, None] * state + grown

def tree_links(parents, keep):
    seq_count, prop_count = parents.shape
    front = jnp.broadcast_to(jnp.arange(-1, keep - 1, dtype=jnp.int32)[None, :], (seq_count, keep))
    parent_ids = jnp.concatenate([front, parents.astype(jnp.int32) + keep], axis=1)
    nodes = keep + prop_count
    links = (parent_ids[:, :, None] == jnp.arange(nodes, dtype=jnp.int32)[None, None, :]).astype(jnp.float32)
    identity = jnp.eye(prop_count, dtype=jnp.float32)[None, :, :]
    ancestry = identity + links[:, keep:, keep:]
    for turn in range(prop_count.bit_length()):
        ancestry = jnp.minimum(jnp.einsum('sij,sjk->sik', ancestry, ancestry, precision=HIGH), 1.0)
    return (links, ancestry)

def tree_conv(buffer, rows, taps, links, keep):
    values = jnp.concatenate([buffer, rows], axis=1).astype(jnp.float32)
    weights = taps.astype(jnp.float32)
    last_tap = weights.shape[0] - 1
    summed = weights[last_tap] * values
    reached = values
    for distance in range(1, last_tap + 1):
        reached = jnp.einsum('sij,sjc->sic', links, reached, precision=HIGH)
        summed = summed + weights[last_tap - distance] * reached
    return jax.nn.silu(summed[:, keep:, :])

def tree_mix(state, post_x, post_b, post_c, rate_rows, z_rows, ancestry, rate_bias, a_rate, d_skip, gain_out, per_group):
    seq_count, prop_count, _ = post_x.shape
    heads, head_dim, state_dim = (state.shape[1], state.shape[2], state.shape[3])
    groups = heads // per_group
    x_heads = post_x.reshape(seq_count, prop_count, heads, head_dim)
    b_groups = post_b.reshape(seq_count, prop_count, groups, state_dim)
    c_groups = post_c.reshape(seq_count, prop_count, groups, state_dim)
    step_size = jax.nn.softplus(rate_rows.astype(jnp.float32) + rate_bias)
    path_decay = jnp.einsum('sij,sjh->sih', ancestry, step_size * a_rate, precision=HIGH)
    c_heads = jnp.repeat(c_groups, per_group, axis=2)
    carried = jnp.einsum('sihn,shpn->sihp', c_heads, state, precision=HIGH) * jnp.exp(path_decay)[:, :, :, None]
    scores = jnp.einsum('sign,sjgn->sgij', c_groups, b_groups, precision=HIGH)
    scores = jnp.repeat(scores, per_group, axis=1)
    decay_t = jnp.transpose(path_decay, (0, 2, 1))
    decay_gap = decay_t[:, :, :, None] - decay_t[:, :, None, :]
    is_live = ancestry[:, None, :, :] > 0.5
    mixing = jnp.where(is_live, jnp.exp(jnp.where(is_live, decay_gap, 0.0)), 0.0)
    mixing = mixing * jnp.transpose(step_size, (0, 2, 1))[:, :, None, :]
    within = jnp.einsum('shij,sjhp->sihp', scores * mixing, x_heads, precision=HIGH)
    heads_out = carried + within + d_skip[None, None, :, None] * x_heads
    heads_out = heads_out.reshape(seq_count, prop_count, heads * head_dim) * jax.nn.silu(z_rows.astype(jnp.float32))
    grouped = heads_out.reshape(seq_count, prop_count, groups, per_group * head_dim)
    grouped = grouped * lax.rsqrt(lax.optimization_barrier(jnp.mean(grouped * grouped, axis=-1, keepdims=True)) + EPS)
    return (grouped.reshape(seq_count, prop_count, heads * head_dim) * gain_out).astype(jnp.bfloat16)

def reference(tokens, parents, accepted, state, conv_x, conv_b, conv_c, path_x, path_b, path_c, path_dt, gain_in, w_x, w_z, w_b, w_c, w_dt, dt_bias, a_log, d_skip, conv_wx, conv_wb, conv_wc, gain_out, w_out):
    seq_count, prop_count, width = tokens.shape
    keep = conv_wx.shape[0] - 1
    flat_rows = tokens.reshape(-1, width).astype(jnp.float32)
    row_scale = lax.rsqrt(lax.optimization_barrier(jnp.sum(flat_rows * flat_rows, axis=1)) / width + EPS)[:, None]
    scaled = (flat_rows * gain_in).astype(jnp.bfloat16)

    def project(weight):
        product = jnp.dot(scaled, weight, preferred_element_type=jnp.float32) * row_scale
        return product.astype(jnp.bfloat16).reshape(seq_count, prop_count, -1)
    x_rows = project(w_x)
    z_rows = project(w_z)
    b_rows = project(w_b)
    c_rows = project(w_c)
    rate_rows = project(w_dt)
    a_rate = -jnp.exp(a_log)
    history_x = jnp.concatenate([conv_x, path_x], axis=1)
    history_b = jnp.concatenate([conv_b, path_b], axis=1)
    history_c = jnp.concatenate([conv_c, path_c], axis=1)
    new_state = replay_state(state, history_x, history_b, path_dt, conv_wx, conv_wb, accepted, dt_bias, a_rate, HPG)
    links, ancestry = tree_links(parents, keep)
    post_x = tree_conv(commit_rows(history_x, accepted, keep), x_rows, conv_wx, links, keep)
    post_b = tree_conv(commit_rows(history_b, accepted, keep), b_rows, conv_wb, links, keep)
    post_c = tree_conv(commit_rows(history_c, accepted, keep), c_rows, conv_wc, links, keep)
    gated = tree_mix(new_state, post_x, post_b, post_c, rate_rows, z_rows, ancestry, dt_bias, a_rate, d_skip, gain_out, HPG)
    block = gated.shape[2] // N_TP
    gated_flat = gated.reshape(-1, gated.shape[2])
    running = jnp.zeros((gated_flat.shape[0], width), jnp.float32)
    for index in range(N_TP):
        term = jnp.dot(gated_flat[:, index * block:(index + 1) * block], w_out[index * block:(index + 1) * block, :], preferred_element_type=jnp.float32)
        rounded = lax.optimization_barrier(term.astype(jnp.bfloat16))
        running = running + rounded.astype(jnp.float32)
    mixed = running.astype(jnp.bfloat16).reshape(seq_count, prop_count, width)
    return (mixed, new_state)
```

```python
import functools

import jax
import jax.numpy as jnp
from jax import lax
from jax.experimental import pallas as pl
from jax.experimental.pallas import tpu as pltpu
from jax.sharding import PartitionSpec as P

HPG = 4
CORES = 2
EPS = 1e-06
HIGH = lax.Precision.HIGHEST
MESH = pl.DeviceIdType.MESH
F32 = jnp.float32
BF16 = jnp.bfloat16
LANES = 128


def inner_size(ranks):
    return max(d for d in range(1, ranks + 1) if ranks % d == 0 and d * d <= ranks)


def dot(a, b):
    return jnp.dot(a, b, preferred_element_type=F32)


def dot_nt(a, b):
    return lax.dot_general(a, b, (((1,), (1,)), ((), ())), preferred_element_type=F32)


def dot_high(a, b):
    return jnp.dot(a, b, precision=HIGH, preferred_element_type=F32)


def silu(x):
    return x * (1.0 / (1.0 + jnp.exp(-x)))


def softplus(x):
    return jnp.maximum(x, 0.0) + jnp.log1p(jnp.exp(-jnp.abs(x)))


def iota(shape, dim):
    return lax.broadcasted_iota(jnp.int32, shape, dim)


class Stream:
    def __init__(self, index, part, near, made, pair, onward, landed):
        self.index = index
        self.part, self.near, self.made = part, near, made
        self.pair, self.onward, self.landed = pair, onward, landed


def scatter_kernel(
    near,
    far,
    chunks,
    heads,
    width,
    tok_ref,
    gain_ref,
    wx_ref,
    wz_ref,
    wb_ref,
    wc_ref,
    wdt_ref,
    x_ref,
    z_ref,
    b_ref,
    c_ref,
    rate_ref,
    wbuf,
    wrate,
    scaled,
    part,
    near_in,
    made,
    pair_in,
    onward,
    far_in,
    side_part,
    side_near,
    side_made,
    side_pair,
    side_onward,
    side_far,
    zpart,
    zpair,
    zonward,
    zfar,
    zfin_out,
    zfin_in,
    w_sems,
    near_s,
    near_r,
    pair_s,
    pair_r,
    far_s,
    far_r,
    zpair_s,
    zpair_r,
    zfar_s,
    zfar_r,
    zfin_s,
    zfin_r,
):
    mine = lax.axis_index("kv")
    column = lax.axis_index("tp")
    my_far = mine // near
    my_near = lax.rem(mine, near)
    partner = my_far + 1 - 2 * lax.rem(my_far, 2)
    half = far // 2
    slab = scaled.shape[2]
    rows = scaled.shape[1]
    ranks = near * far
    wx_cols = wx_ref.shape[1] // chunks
    wb_cols = wb_ref.shape[1] // chunks
    first = 2 * wx_cols + wb_cols
    seqs = tok_ref.shape[1] // ranks

    loads = []
    for g in range(chunks):
        at = 0
        for k, (ref, cols) in enumerate(
            ((wx_ref, wx_cols), (wz_ref, wx_cols), (wb_ref, wb_cols), (wc_ref, wb_cols))
        ):
            copy = pltpu.make_async_copy(
                ref.at[:, pl.ds(g * cols, cols)], wbuf.at[g, :, pl.ds(at, cols)], w_sems.at[g, k]
            )
            copy.start()
            loads.append(copy)
            at += cols
    rate_load = pltpu.make_async_copy(
        wdt_ref.at[
            pl.ds(pl.multiple_of(column * heads, heads), heads),
            pl.ds(pl.multiple_of(mine * slab, slab), slab),
        ],
        wrate,
        w_sems.at[chunks, 0],
    )
    rate_load.start()

    def place(home, jump, step_near):
        return lax.rem(home + 2 * jump, far) * near + lax.rem(my_near + step_near, near)

    barrier = pltpu.get_barrier_semaphore()
    peers = [place(my_far, 0, step) for step in range(1, near)]
    peers = peers + [place(partner, 0, 0)]
    peers = peers + [place(my_far, jump, 0) for jump in range(1, half)]
    for peer in peers:
        pl.semaphore_signal(barrier, inc=1, device_id=(peer, column), device_id_type=MESH)

    rate_load.wait()
    gain = gain_ref[:, pl.ds(pl.multiple_of(mine * slab, slab), slab)]
    rate_w = wrate[...]

    @pl.loop(0, ranks)
    def _(d):
        tokens = tok_ref[:, pl.ds(pl.multiple_of(d * seqs, seqs), seqs), :].astype(F32).reshape(rows, slab)
        block = (tokens * gain).astype(BF16)
        scaled[d] = block
        squares = jnp.sum(tokens * tokens, axis=1, keepdims=True)
        rates = dot_nt(block, rate_w)
        side_part[d, :, 0:heads] = rates.astype(BF16)
        side_part[d, :, heads : heads + 1] = squares.astype(BF16)

    def multiply(g):
        for copy in loads[4 * g : 4 * g + 4]:
            copy.wait()

        @pl.loop(0, ranks // 2)
        def _(turn):
            block = scaled[pl.ds(2 * turn, 2)].reshape(2 * rows, slab)
            both = dot(block, wbuf[g]).astype(BF16)
            for k in range(2):
                part[g, 2 * turn + k] = both[k * rows : (k + 1) * rows, :first]
                zpart[g, 2 * turn + k] = both[k * rows : (k + 1) * rows, first:]

    order = [(jump, kind) for jump in list(range(1, half)) + [0] for kind in range(2)]
    turns = len(order)
    homes = (partner, my_far)
    side = Stream(chunks, side_part, side_near, side_made, side_pair, side_onward, side_far)
    streams = []
    for g in range(chunks):
        stream = Stream(
            g, part.at[g], near_in.at[g], made.at[g], pair_in.at[g], onward.at[g], far_in.at[g]
        )
        streams.append([side, stream] if g == 0 else [stream])

    copies = []
    waits = {}

    def send(key, source, landing, send_sem, recv_sem, target):
        copy = pltpu.make_async_remote_copy(
            src_ref=source,
            dst_ref=landing,
            send_sem=send_sem,
            recv_sem=recv_sem,
            device_id=(target, column),
            device_id_type=MESH,
        )
        copy.start()
        copies.append(copy)
        waits[key] = copy

    def start_near(q):
        g, t = q // turns, q % turns
        jump, kind = order[t]
        slot = 2 * jump + kind
        for step in range(1, near):
            for s in streams[g]:
                send(
                    ("near", s.index, slot, step),
                    s.part.at[place(homes[kind], jump, step)],
                    s.near.at[slot, step - 1],
                    near_s.at[s.index, slot, step - 1],
                    near_r.at[s.index, slot, step - 1],
                    place(my_far, 0, step),
                )

    def start_zpair(g):
        for jump in list(range(1, half)) + [0]:
            for step in range(near):
                send(
                    ("zpair", g, jump, step),
                    zpart.at[g, place(partner, jump, step)],
                    zpair.at[g, jump, step],
                    zpair_s.at[g, jump, step],
                    zpair_r.at[g, jump, step],
                    place(partner, 0, 0),
                )

    def sum_of(first_term, others):
        total = first_term.astype(F32)
        for other in others:
            total = total + other.astype(F32)
        return total

    def near_terms(s, slot):
        return [s.near[slot, step - 1] for step in range(1, near)]

    def step_kind0(g, jump):
        slot = 2 * jump
        for s in streams[g]:
            for step in range(1, near):
                waits["near", s.index, slot, step].wait_recv()
            s.made[jump] = sum_of(s.part[place(partner, jump, 0)], near_terms(s, slot)).astype(BF16)
            send(
                ("pair", s.index, jump),
                s.made.at[jump],
                s.pair.at[jump],
                pair_s.at[s.index, jump],
                pair_r.at[s.index, jump],
                place(partner, 0, 0),
            )

    def step_kind1(g, jump):
        slot = 2 * jump + 1
        for s in streams[g]:
            for step in range(1, near):
                waits["near", s.index, slot, step].wait_recv()
            if jump == 0:
                continue
            waits["pair", s.index, jump].wait_recv()
            s.onward[jump - 1] = sum_of(
                s.part[place(my_far, jump, 0)], near_terms(s, slot) + [s.pair[jump]]
            ).astype(BF16)
            send(
                ("far", s.index, jump),
                s.onward.at[jump - 1],
                s.landed.at[jump - 1],
                far_s.at[s.index, jump - 1],
                far_r.at[s.index, jump - 1],
                place(my_far, jump, 0),
            )

    def z_onward(g):
        for jump in range(1, half):
            for step in range(near):
                waits["zpair", g, jump, step].wait_recv()
                zonward[g, jump - 1, step] = sum_of(
                    zpart[g, place(my_far, jump, step)], [zpair[g, jump, step]]
                ).astype(BF16)
                send(
                    ("zfar", g, jump, step),
                    zonward.at[g, jump - 1, step],
                    zfar.at[g, jump - 1, step],
                    zfar_s.at[g, jump - 1, step],
                    zfar_r.at[g, jump - 1, step],
                    place(my_far, jump, 0),
                )

    def z_terms(g, step):
        return [zpair[g, 0, step]] + [zfar[g, jump - 1, step] for jump in range(1, half)]

    def z_last(g):
        for step in range(near):
            waits["zpair", g, 0, step].wait_recv()
            for jump in range(1, half):
                waits["zfar", g, jump, step].wait_recv()
        for step in range(1, near):
            zfin_out[g, step - 1] = sum_of(
                zpart[g, place(my_far, 0, step)], z_terms(g, step)
            ).astype(BF16)
            send(
                ("zfin", g, step),
                zfin_out.at[g, step - 1],
                zfin_in.at[g, step - 1],
                zfin_s.at[g, step - 1],
                zfin_r.at[g, step - 1],
                place(my_far, 0, step),
            )

    scale = []

    def finish(g):
        for s in streams[g]:
            waits["pair", s.index, 0].wait_recv()
            for jump in range(1, half):
                waits["far", s.index, jump].wait_recv()
            total = sum_of(
                s.part[mine],
                near_terms(s, 1) + [s.pair[0]] + [s.landed[jump - 1] for jump in range(1, half)],
            )
            if s is side:
                scale.append(lax.rsqrt(total[:, heads : heads + 1] / width + EPS))
                rate_ref[...] = (total[:, 0:heads] * scale[0]).astype(BF16)
            else:
                total = (total * scale[0]).astype(BF16)
                x_ref[:, g * wx_cols : (g + 1) * wx_cols] = total[:, :wx_cols]
                z_ref[:, g * wx_cols : (g + 1) * wx_cols] = total[:, wx_cols : 2 * wx_cols]
                b_ref[:, g * wb_cols : (g + 1) * wb_cols] = total[:, 2 * wx_cols :]
        for step in range(1, near):
            waits["zfin", g, step].wait_recv()
        total = sum_of(
            zpart[g, mine], z_terms(g, 0) + [zfin_in[g, step - 1] for step in range(1, near)]
        )
        c_ref[:, g * wb_cols : (g + 1) * wb_cols] = (total * scale[0]).astype(BF16)

    ahead = 3
    multiply(0)
    pl.semaphore_wait(barrier, len(peers))
    for q in range(min(ahead, chunks * turns)):
        if q > 0 and q % turns == 0:
            multiply(q // turns)
        start_near(q)
    start_zpair(0)
    for g in range(chunks):
        if g + 1 < chunks and turns > ahead:
            multiply(g + 1)
        for t, (jump, kind) in enumerate(order):
            if kind == 0:
                step_kind0(g, jump)
            else:
                step_kind1(g, jump)
            if g * turns + t + ahead < chunks * turns:
                start_near(g * turns + t + ahead)
            if t == 0:
                z_onward(g)
            if t == 1 and g + 1 < chunks:
                start_zpair(g + 1)
            if t == turns - 2:
                z_last(g)
        if g > 0:
            finish(g - 1)
    finish(chunks - 1)
    for copy in copies:
        copy.wait_send()


def scatter_rows(tokens, gain, w_x, w_z, w_b, w_c, w_dt, heads, ranks, chunks):
    props, all_seqs, slab = tokens.shape
    rows = props * all_seqs // ranks
    near = inner_size(ranks)
    far = ranks // near
    half = far // 2
    xc = w_x.shape[1] // chunks
    bc = w_b.shape[1] // chunks
    wide = 2 * xc + bc
    vmem = pl.BlockSpec(memory_space=pltpu.VMEM)
    hbm = pl.BlockSpec(memory_space=pl.ANY)
    dma = pltpu.SemaphoreType.DMA

    def buf(*shape):
        return pltpu.VMEM(shape, BF16)

    scratch = [
        buf(chunks, slab, wide + bc),
        buf(heads, slab),
        buf(ranks, rows, slab),
        buf(chunks, ranks, rows, wide),
        buf(chunks, far, near - 1, rows, wide),
        buf(chunks, half, rows, wide),
        buf(chunks, half, rows, wide),
        buf(chunks, half - 1, rows, wide),
        buf(chunks, half - 1, rows, wide),
        buf(ranks, rows, LANES),
        buf(far, near - 1, rows, LANES),
        buf(half, rows, LANES),
        buf(half, rows, LANES),
        buf(half - 1, rows, LANES),
        buf(half - 1, rows, LANES),
        buf(chunks, ranks, rows, bc),
        buf(chunks, half, near, rows, bc),
        buf(chunks, half - 1, near, rows, bc),
        buf(chunks, half - 1, near, rows, bc),
        buf(chunks, near - 1, rows, bc),
        buf(chunks, near - 1, rows, bc),
        dma((chunks + 1, 4)),
    ]
    for shape in (
        (chunks + 1, far, near - 1),
        (chunks + 1, half),
        (chunks + 1, half - 1),
        (chunks, half, near),
        (chunks, half - 1, near),
        (chunks, near - 1),
    ):
        scratch += [dma(shape), dma(shape)]
    return pl.pallas_call(
        functools.partial(scatter_kernel, near, far, chunks, heads, gain.shape[1]),
        out_shape=(
            jax.ShapeDtypeStruct((rows, w_x.shape[1]), BF16),
            jax.ShapeDtypeStruct((rows, w_z.shape[1]), BF16),
            jax.ShapeDtypeStruct((rows, w_b.shape[1]), BF16),
            jax.ShapeDtypeStruct((rows, w_c.shape[1]), BF16),
            jax.ShapeDtypeStruct((rows, heads), BF16),
        ),
        in_specs=[vmem, vmem, hbm, hbm, hbm, hbm, hbm],
        out_specs=(vmem,) * 5,
        scratch_shapes=scratch,
        compiler_params=pltpu.CompilerParams(collective_id=0, has_side_effects=True),
        name="scatter",
    )(tokens, gain, w_x, w_z, w_b, w_c, w_dt)


def spread(values, g, lanes):
    head = lanes // HPG
    lane = iota((1, lanes), 1)
    out = values[:, HPG * g : HPG * g + 1]
    for i in range(1, HPG):
        out = jnp.where(lane >= i * head, values[:, HPG * g + i : HPG * g + i + 1], out)
    return out


def mix_kernel(
    x_ref,
    z_ref,
    b_ref,
    c_ref,
    rate_ref,
    parents_ref,
    accepted_ref,
    state_ref,
    conv_x_ref,
    conv_b_ref,
    conv_c_ref,
    path_x_ref,
    path_b_ref,
    path_c_ref,
    path_dt_ref,
    bias_ref,
    alog_ref,
    skip_ref,
    wx_ref,
    wb_ref,
    wc_ref,
    gain_ref,
    gated_ref,
    new_ref,
    hist,
    state_vm,
    new_vm,
    new_bf,
    in_sems,
    out_sems,
):
    seqs, heads, head_dim, state_dim = state_ref.shape
    groups = heads // HPG
    props = parents_ref.shape[1]
    rows = seqs * props
    keep, path_len = conv_x_ref.shape[0], path_x_ref.shape[0]
    taps = keep + 1
    held = keep + path_len
    hrows, prows = held * seqs, path_len * seqs
    xc, bc = HPG * head_dim, state_dim
    wide = xc + 2 * bc
    low = seqs - 1
    shift = seqs.bit_length() - 1

    loads = []
    for g in range(groups):
        copy = pltpu.make_async_copy(
            state_ref.at[:, pl.ds(HPG * g, HPG)], state_vm.at[g], in_sems.at[g]
        )
        copy.start()
        loads.append(copy)

    for g in range(groups):
        at = 0
        for conv, path, cols in (
            (conv_x_ref, path_x_ref, xc),
            (conv_b_ref, path_b_ref, bc),
            (conv_c_ref, path_c_ref, bc),
        ):
            span = slice(g * cols, (g + 1) * cols)
            top = conv[:, :, span].astype(F32).reshape(keep * seqs, cols)
            end = path[:, :, span].astype(F32).reshape(prows, cols)
            hist[g, :, at : at + cols] = jnp.concatenate([top, end], axis=0).astype(BF16)
            at += cols

    def tap(k, g, parts):
        refs = ((wx_ref, xc), (wb_ref, bc), (wc_ref, bc))
        return jnp.concatenate(
            [ref[k : k + 1, g * cols : (g + 1) * cols].astype(F32) for ref, cols in refs[:parts]],
            axis=1,
        )

    bias = bias_ref[...]
    a_rate = -jnp.exp(alog_ref[...])
    eye = iota((seqs, seqs), 0) == iota((seqs, seqs), 1)
    accepted = jnp.sum(
        jnp.where(eye, accepted_ref[...].astype(F32), 0.0), axis=1, keepdims=True
    )

    acc_path = jnp.concatenate([accepted] * path_len, axis=0)
    step_of = lax.shift_right_logical(iota((prows, 1), 0), shift).astype(F32)
    live = (step_of < acc_path).astype(F32)
    path_step = softplus(path_dt_ref[...].astype(F32).reshape(prows, heads) + bias)
    log_decay = path_step * a_rate * live
    pr, pc = iota((prows, prows), 0), iota((prows, prows), 1)
    same = (pr & low) == (pc & low)
    later = jnp.where(same & (pc > pr), 1.0, 0.0)
    tail = dot_high(later, log_decay)
    every = jnp.where(iota((seqs, prows), 0) == (iota((seqs, prows), 1) & low), 1.0, 0.0)
    overall = jnp.exp(dot_high(every, log_decay))
    weights = live * jnp.exp(tail) * path_step
    block_mask = (iota((prows, seqs * bc), 0) & low) == lax.shift_right_logical(
        iota((prows, seqs * bc), 1), bc.bit_length() - 1
    )

    for g in range(groups):
        values = hist[g, :, 0 : xc + bc].astype(F32)
        summed = tap(0, g, 2) * values[0:prows]
        for k in range(1, taps):
            summed = summed + tap(k, g, 2) * values[k * seqs : k * seqs + prows]
        post = silu(summed)
        left = (post[:, :xc] * spread(weights, g, xc)).T.astype(BF16)
        right = jnp.where(block_mask, jnp.concatenate([post[:, xc:]] * seqs, axis=1), 0.0)
        grown = dot(left, right.astype(BF16))
        loads[g].wait()
        for s in range(seqs):
            for i in range(HPG):
                h = HPG * g + i
                fresh = (
                    overall[s : s + 1, h : h + 1] * state_vm[g, s, i]
                    + grown[i * head_dim : (i + 1) * head_dim, s * bc : (s + 1) * bc]
                )
                new_vm[g, s, i] = fresh
                new_bf[g, i * head_dim : (i + 1) * head_dim, s * bc : (s + 1) * bc] = fresh.astype(
                    BF16
                )
        pltpu.make_async_copy(
            new_vm.at[g], new_ref.at[:, pl.ds(HPG * g, HPG)], out_sems.at[g]
        ).start()

    parents = parents_ref[...].astype(F32)
    parent = jnp.concatenate([parents[:, i : i + 1] for i in range(props)], axis=0)
    acc_rows = jnp.concatenate([accepted] * props, axis=0)
    seq_of = (iota((rows, 1), 0) & low).astype(F32)
    in_tree = parent >= 0.0
    hist_at = jnp.where(in_tree, -1.0, (acc_rows + (keep - 1)) * seqs + seq_of)
    prop_at = jnp.where(in_tree, parent * seqs + seq_of, -1.0)
    link_p = iota((rows, rows), 1).astype(F32) == prop_at
    link_h = iota((rows, hrows), 1).astype(F32) == hist_at
    up_p = jnp.where(link_p, 1.0, 0.0).astype(BF16)
    up_h = jnp.where(link_h, 1.0, 0.0).astype(BF16)
    back = jnp.where(
        iota((hrows, hrows), 1) == iota((hrows, hrows), 0) - seqs, 1.0, 0.0
    ).astype(BF16)
    ups_p, ups_h = [up_p], [up_h]
    for _ in range(1, taps - 1):
        last_p, last_h = ups_p[-1], ups_h[-1]
        ups_p.append(dot(last_p, up_p).astype(BF16))
        ups_h.append((dot(last_p, up_h) + dot(last_h, back)).astype(BF16))
    all_p = jnp.concatenate(ups_p, axis=0)
    all_h = jnp.concatenate(ups_h, axis=0)
    self_at = iota((rows, rows), 0) == iota((rows, rows), 1)
    tree = jnp.where(link_p | self_at, 1.0, 0.0)
    for _ in range((props - 1).bit_length()):
        some = tree.astype(BF16)
        tree = jnp.minimum(dot(some, some), 1.0)
    above = tree > 0.5

    step_size = softplus(rate_ref[...].astype(F32) + bias)
    decay = dot_high(tree, step_size * a_rate)
    decay_t = decay.T
    step_t = step_size.T
    carried_scale = jnp.exp(decay)
    own = (iota((rows, seqs * bc), 0) & low) == lax.shift_right_logical(
        iota((rows, seqs * bc), 1), bc.bit_length() - 1
    )
    lane = iota((1, xc), 1)

    for g in range(groups):
        here = jnp.concatenate(
            [
                x_ref[:, g * xc : (g + 1) * xc],
                b_ref[:, g * bc : (g + 1) * bc],
                c_ref[:, g * bc : (g + 1) * bc],
            ],
            axis=1,
        )
        summed = tap(taps - 1, g, 3) * here.astype(F32)
        reached = dot(all_p, here) + dot(all_h, hist[g])
        for k in range(1, taps):
            summed = summed + tap(taps - 1 - k, g, 3) * reached[(k - 1) * rows : k * rows]
        post = silu(summed)
        post_x = post[:, :xc]
        post_b = post[:, xc : xc + bc].astype(BF16)
        post_c = post[:, xc + bc :]
        scores = dot_nt(post_c.astype(BF16), post_b)
        out = jnp.zeros((rows, xc), F32)
        for i in range(HPG):
            h = HPG * g + i
            gap = decay[:, h : h + 1] - decay_t[h : h + 1, :]
            mixing = jnp.where(above, jnp.exp(jnp.where(above, gap, 0.0)), 0.0)
            mixing = scores * mixing * step_t[h : h + 1, :]
            mine = (lane >= i * head_dim) & (lane < (i + 1) * head_dim)
            out = out + dot(mixing.astype(BF16), jnp.where(mine, post_x, 0.0).astype(BF16))
        wide_c = jnp.where(own, jnp.concatenate([post_c] * seqs, axis=1), 0.0).astype(BF16)
        carried = dot_nt(wide_c, new_bf[g])
        out = out + carried * spread(carried_scale, g, xc) + spread(skip_ref[...], g, xc) * post_x
        out = out * silu(z_ref[:, g * xc : (g + 1) * xc].astype(F32))
        out = out * lax.rsqrt(jnp.mean(out * out, axis=1, keepdims=True) + EPS)
        gated_ref[:, g * xc : (g + 1) * xc] = (out * gain_ref[:, g * xc : (g + 1) * xc]).astype(
            BF16
        )
    for g in range(groups):
        pltpu.make_async_copy(
            new_vm.at[g], new_ref.at[:, pl.ds(HPG * g, HPG)], out_sems.at[g]
        ).wait()


def mix(projected, parents, accepted, state, conv, path, path_dt, small, taps, gain_out):
    rows, inner = projected[0].shape
    seqs, heads, head_dim, state_dim = state.shape
    groups = heads // HPG
    held = conv[0].shape[0] + path[0].shape[0]
    vmem = pl.BlockSpec(memory_space=pltpu.VMEM)
    hbm = pl.BlockSpec(memory_space=pl.ANY)
    return pl.pallas_call(
        mix_kernel,
        out_shape=(
            jax.ShapeDtypeStruct((rows, inner), BF16),
            jax.ShapeDtypeStruct(state.shape, F32),
        ),
        in_specs=[vmem] * 7 + [hbm] + [vmem] * 14,
        out_specs=(vmem, hbm),
        scratch_shapes=[
            pltpu.VMEM((groups, held * seqs, HPG * head_dim + 2 * state_dim), BF16),
            pltpu.VMEM((groups, seqs, HPG, head_dim, state_dim), F32),
            pltpu.VMEM((groups, seqs, HPG, head_dim, state_dim), F32),
            pltpu.VMEM((groups, HPG * head_dim, seqs * state_dim), BF16),
            pltpu.SemaphoreType.DMA((groups,)),
            pltpu.SemaphoreType.DMA((groups,)),
        ],
        name="mix",
    )(*projected, parents, accepted, state, *conv, *path, path_dt, *small, *taps, gain_out)


def out_kernel(
    near,
    far,
    ratio,
    cores,
    gated_ref,
    w_ref,
    mixed_ref,
    w_vm,
    gathered,
    terms,
    sibling_in,
    paired,
    column_in,
    done,
    landed,
    w_sem,
    gather_s,
    gather_r,
    sib_s,
    sib_r,
    col_s,
    col_r,
    done_s,
    done_r,
):
    mine = lax.axis_index("kv")
    column = lax.axis_index("tp")
    blocks = lax.axis_size("tp")
    ranks = near * far
    half = far // 2
    depth = blocks // cores
    my_far = mine // near
    my_near = lax.rem(mine, near)
    partner = my_far + 1 - 2 * lax.rem(my_far, 2)
    core = lax.rem(column, cores)
    level = column // cores
    owner = mine // ratio
    spot = lax.rem(mine, ratio)
    owner_level = owner // cores
    owner_core = lax.rem(owner, cores)
    slab = w_ref.shape[1]

    load = pltpu.make_async_copy(w_ref, w_vm, w_sem)
    load.start()

    def place(home, jump, step_near):
        return lax.rem(home + 2 * jump, far) * near + lax.rem(my_near + step_near, near)

    barrier = pltpu.get_barrier_semaphore()

    def greet(target):
        pl.semaphore_signal(barrier, inc=1, device_id=target, device_id_type=MESH)

    count = 0
    for peer in (
        [place(my_far, jump, 0) for jump in range(1, half)]
        + [place(partner, 0, 0)]
        + [place(my_far, 0, step) for step in range(1, near)]
    ):
        greet((peer, column))
        count += 1
    for other in range(1, cores):
        greet((mine, level * cores + lax.rem(core + other, cores)))
        count += 1

    @pl.when(level != owner_level)
    def _():
        greet((mine, owner_level * cores + core))

    for up in range(1, depth):

        @pl.when(level == owner_level)
        def _():
            greet((mine, lax.rem(level + up, depth) * cores + core))

    for n in range(ratio):
        for c in range(cores):
            source = column * ratio + n

            @pl.when(jnp.logical_or(source != mine, c != core))
            def _():
                greet((source, level * cores + c))

    @pl.when(level != owner_level)
    def _():
        pl.semaphore_wait(barrier, count + 1)

    @pl.when(jnp.logical_and(level == owner_level, core != owner_core))
    def _():
        pl.semaphore_wait(barrier, count + depth - 1 + ranks)

    @pl.when(jnp.logical_and(level == owner_level, core == owner_core))
    def _():
        pl.semaphore_wait(barrier, count + depth - 1 + ranks - 1)

    index = {}
    for home in range(2):
        for jump in range(half):
            for step in range(near):
                index[jump, home, step] = len(index)
    homes = (my_far, partner)

    def origin(key):
        jump, home, step = key
        return lax.rem(homes[home] + 2 * (half - jump) % far, far) * near + lax.rem(
            my_near + near - step, near
        )

    copies = []
    waits = {}

    def gather(key, source, target):
        k = index[key]
        copy = pltpu.make_async_remote_copy(
            src_ref=source,
            dst_ref=gathered.at[k],
            send_sem=gather_s.at[k],
            recv_sem=gather_r.at[k],
            device_id=(target, column),
            device_id_type=MESH,
        )
        copy.start()
        copies.append(copy)
        waits[key] = copy

    def block_ref(key):
        return gated_ref if key == (0, 0, 0) else gathered.at[index[key]]

    for jump in range(1, half):
        gather((jump, 0, 0), gated_ref, place(my_far, jump, 0))
    gather((0, 1, 0), gated_ref, place(partner, 0, 0))
    for step in range(1, near):
        gather((0, 0, step), gated_ref, place(my_far, 0, step))
    load.wait()

    def multiply(key):
        if key != (0, 0, 0):
            waits[key].wait_recv()
        jump, home, step = key
        if home == 0 and jump > 0 and step == 0:
            gather((jump, 1, 0), block_ref(key), place(partner, 0, 0))
        if step == 0 and (home, jump) != (0, 0):
            for s in range(1, near):
                gather((jump, home, s), block_ref(key), place(my_far, 0, s))
        terms[index[key]] = dot(block_ref(key)[...], w_vm[...]).astype(BF16)

    order = [(0, 0, 0)] + [(jump, 0, 0) for jump in range(1, half)]
    order += [(0, 1, 0)] + [(0, 0, step) for step in range(1, near)]
    order += [(jump, 1, 0) for jump in range(1, half)]
    order += [(jump, 0, step) for jump in range(1, half) for step in range(1, near)]
    order += [(jump, 1, step) for jump in range(half) for step in range(1, near)]
    batches = [order[at : at + cores] for at in range(0, len(order), cores)]

    def pick(keys, which):
        out = index[keys[0]]
        for k in range(1, cores):
            out = jnp.where(which == k, index[keys[k]], out)
        return out

    def pick_origin(keys, which):
        out = origin(keys[0])
        for k in range(1, cores):
            out = jnp.where(which == k, origin(keys[k]), out)
        return out

    def sibling_copy(n, other):
        target = lax.rem(core + other, cores)
        return pltpu.make_async_remote_copy(
            src_ref=terms.at[pick(batches[n], target)],
            dst_ref=sibling_in.at[n, other - 1],
            send_sem=sib_s.at[n, other - 1],
            recv_sem=sib_r.at[n, other - 1],
            device_id=(mine, level * cores + target),
            device_id_type=MESH,
        )

    def column_copy(n, up):
        return pltpu.make_async_remote_copy(
            src_ref=paired.at[n],
            dst_ref=column_in.at[n, up - 1],
            send_sem=col_s.at[n],
            recv_sem=col_r.at[n, up - 1],
            device_id=(mine, owner_level * cores + core),
            device_id_type=MESH,
        )

    def done_copy(n):
        return pltpu.make_async_remote_copy(
            src_ref=done.at[n],
            dst_ref=landed.at[spot],
            send_sem=done_s.at[n],
            recv_sem=done_r.at[spot],
            device_id=(pick_origin(batches[n], core), owner),
            device_id_type=MESH,
        )

    def stays(n):
        if (0, 0, 0) not in batches[n]:
            return None
        return jnp.logical_and(core == batches[n].index((0, 0, 0)), owner == column)

    def level_gap():
        return lax.rem(level - owner_level + depth, depth)

    def pair_up(n):
        total = terms[pick(batches[n], core)].astype(F32)
        for other in range(1, cores):
            sibling_copy(n, other).wait_recv()
            total = total + sibling_in[n, other - 1].astype(F32)
        paired[n] = total.astype(BF16)
        for up in range(1, depth):

            @pl.when(level_gap() == up)
            def _():
                column_copy(n, up).start()

    def finish(n):
        @pl.when(level == owner_level)
        def _():
            total = paired[n].astype(F32)
            for up in range(1, depth):
                column_copy(n, up).wait_recv()
                total = total + column_in[n, up - 1].astype(F32)
            done[n] = total.astype(BF16)
            here = stays(n)
            if here is None:
                done_copy(n).start()
            else:

                @pl.when(here)
                def _():
                    landed[spot] = done[n]

                @pl.when(jnp.logical_not(here))
                def _():
                    done_copy(n).start()

    for n, keys in enumerate(batches):
        for key in keys:
            multiply(key)
        for other in range(1, cores):
            sibling_copy(n, other).start()
        if n >= 1:
            pair_up(n - 1)
        if n >= 2:
            finish(n - 2)
    last = len(batches) - 1
    pair_up(last)
    if last >= 1:
        finish(last - 1)
    finish(last)

    for n in range(ratio):
        source = column * ratio + n
        local = jnp.logical_and(source == mine, core == batches[0].index((0, 0, 0)))

        @pl.when(jnp.logical_not(local))
        def _():
            pltpu.make_async_remote_copy(
                src_ref=done.at[0],
                dst_ref=landed.at[n],
                send_sem=done_s.at[0],
                recv_sem=done_r.at[n],
                device_id=(source, lax.rem(column + 1, blocks)),
                device_id_type=MESH,
            ).wait_recv()

        mixed_ref[:, n * slab : (n + 1) * slab] = landed[n]

    for copy in copies:
        copy.wait_send()
    for n in range(len(batches)):
        for other in range(1, cores):
            sibling_copy(n, other).wait_send()

        @pl.when(level != owner_level)
        def _():
            column_copy(n, 1).wait_send()

        @pl.when(level == owner_level)
        def _():
            here = stays(n)
            if here is None:
                done_copy(n).wait_send()
            else:

                @pl.when(jnp.logical_not(here))
                def _():
                    done_copy(n).wait_send()


def project_out(gated, w_out, ranks, blocks):
    rows = gated.shape[0]
    inner, slab = w_out.shape
    near = inner_size(ranks)
    far = ranks // near
    ratio = ranks // blocks
    depth = blocks // CORES
    batches = ranks // CORES
    vmem = pl.BlockSpec(memory_space=pltpu.VMEM)
    hbm = pl.BlockSpec(memory_space=pl.ANY)
    dma = pltpu.SemaphoreType.DMA
    return pl.pallas_call(
        functools.partial(out_kernel, near, far, ratio, CORES),
        out_shape=jax.ShapeDtypeStruct((rows, ratio * slab), BF16),
        in_specs=[vmem, hbm],
        out_specs=vmem,
        scratch_shapes=[
            pltpu.VMEM((inner, slab), BF16),
            pltpu.VMEM((ranks, rows, inner), BF16),
            pltpu.VMEM((ranks, rows, slab), BF16),
            pltpu.VMEM((batches, CORES - 1, rows, slab), BF16),
            pltpu.VMEM((batches, rows, slab), BF16),
            pltpu.VMEM((batches, depth - 1, rows, slab), BF16),
            pltpu.VMEM((batches, rows, slab), BF16),
            pltpu.VMEM((ratio, rows, slab), BF16),
            dma(()),
            dma((ranks,)),
            dma((ranks,)),
            dma((batches, CORES - 1)),
            dma((batches, CORES - 1)),
            dma((batches,)),
            dma((batches, depth - 1)),
            dma((batches,)),
            dma((ratio,)),
        ],
        compiler_params=pltpu.CompilerParams(collective_id=1, has_side_effects=True),
        name="project_out",
    )(gated, w_out)


def shards(
    tokens,
    parents,
    accepted,
    state,
    conv_x,
    conv_b,
    conv_c,
    path_x,
    path_b,
    path_c,
    path_dt,
    gain_in,
    w_x,
    w_z,
    w_b,
    w_c,
    w_dt,
    dt_bias,
    a_log,
    d_skip,
    conv_wx,
    conv_wb,
    conv_wc,
    gain_out,
    w_out,
):
    ranks = lax.axis_size("kv")
    blocks = lax.axis_size("tp")
    heads = dt_bias.shape[0]

    def front(array):
        return jnp.swapaxes(array, 0, 1)

    projected = scatter_rows(
        front(tokens),
        gain_in[None, :],
        w_x,
        w_z,
        w_b,
        w_c,
        w_dt.T,
        heads,
        ranks,
        heads // HPG,
    )
    gated, new_state = mix(
        projected,
        parents,
        accepted[None, :],
        state,
        (front(conv_x), front(conv_b), front(conv_c)),
        (front(path_x), front(path_b), front(path_c)),
        front(path_dt),
        (dt_bias[None, :], a_log[None, :], d_skip[None, :]),
        (conv_wx, conv_wb, conv_wc),
        gain_out[None, :],
    )
    summed = project_out(gated, w_out, ranks, blocks)
    seqs, props = parents.shape
    mixed = front(summed.reshape(props, seqs, summed.shape[1]))
    return (mixed, new_state)


def solution(mesh):
    return jax.shard_map(
        shards,
        mesh=mesh,
        in_specs=(
            P(None, None, "kv"),
            P("kv", None),
            P("kv"),
            P("kv", "tp", None, None),
            P("kv", None, "tp"),
            P("kv", None, "tp"),
            P("kv", None, "tp"),
            P("kv", None, "tp"),
            P("kv", None, "tp"),
            P("kv", None, "tp"),
            P("kv", None, "tp"),
            P(),
            P("kv", "tp"),
            P("kv", "tp"),
            P("kv", "tp"),
            P("kv", "tp"),
            P(),
            P("tp"),
            P("tp"),
            P("tp"),
            P(None, "tp"),
            P(None, "tp"),
            P(None, "tp"),
            P("tp"),
            P("tp", "kv"),
        ),
        out_specs=(P("kv", None, "tp"), P("kv", "tp", None, None)),
        check_vma=False,
    )
```

```python
import functools

import jax
import jax.numpy as jnp
from jax import lax
from jax.experimental import pallas as pl
from jax.experimental.pallas import tpu as pltpu
from jax.sharding import PartitionSpec as P

HPG = 4
CORES = 2
EPS = 1e-06
HIGH = lax.Precision.HIGHEST
MESH = pl.DeviceIdType.MESH
F32 = jnp.float32
BF16 = jnp.bfloat16
LANES = 128
AHEAD = 3


def inner_size(ranks):
    return max(d for d in range(1, ranks + 1) if ranks % d == 0 and d * d <= ranks)


def dot(a, b):
    return jnp.dot(a, b, preferred_element_type=F32)


def dot_nt(a, b):
    return lax.dot_general(a, b, (((1,), (1,)), ((), ())), preferred_element_type=F32)


def dot_high(a, b):
    return jnp.dot(a, b, precision=HIGH, preferred_element_type=F32)


def silu(x):
    return x * (1.0 / (1.0 + jnp.exp(-x)))


def softplus(x):
    return jnp.maximum(x, 0.0) + jnp.log1p(jnp.exp(-jnp.abs(x)))


def iota(shape, dim):
    return lax.broadcasted_iota(jnp.int32, shape, dim)


class Stream:
    def __init__(self, index, part, near, made, pair, onward, landed):
        self.index = index
        self.part, self.near, self.made = part, near, made
        self.pair, self.onward, self.landed = pair, onward, landed


class Names:
    def __init__(self, names, refs):
        self.__dict__.update(zip(names, refs, strict=True))


def spread(values, g, lanes):
    head = lanes // HPG
    lane = iota((1, lanes), 1)
    out = values[:, HPG * g : HPG * g + 1]
    for i in range(1, HPG):
        out = jnp.where(lane >= i * head, values[:, HPG * g + i : HPG * g + i + 1], out)
    return out


def sum_of(first_term, others):
    total = first_term.astype(F32)
    for other in others:
        total = total + other.astype(F32)
    return total


def mixer_kernel(names, near, far, chunks, ratio, *refs):
    r = Names(names, refs)
    mine = lax.axis_index("kv")
    column = lax.axis_index("tp")
    blocks = lax.axis_size("tp")
    ranks = near * far
    half = far // 2
    depth = blocks // CORES
    my_far = mine // near
    my_near = lax.rem(mine, near)
    partner = my_far + 1 - 2 * lax.rem(my_far, 2)
    core = lax.rem(column, CORES)
    level = column // CORES
    owner = mine // ratio
    spot = lax.rem(mine, ratio)
    owner_level = owner // CORES
    owner_core = lax.rem(owner, CORES)
    slab = r.scaled.shape[2]
    rows = r.scaled.shape[1]
    seqs, heads, head_dim, state_dim = r.state.shape
    props = r.parents.shape[1]
    width = r.gain_in.shape[1]
    keep, path_len = r.conv_x.shape[0], r.path_x.shape[0]
    taps = keep + 1
    hrows, prows = (keep + path_len) * seqs, path_len * seqs
    xc, bc = HPG * head_dim, state_dim
    first = 2 * xc + bc
    out_slab = r.w_out.shape[1]
    low = seqs - 1
    shift = seqs.bit_length() - 1
    bc_shift = bc.bit_length() - 1

    def place(home, jump, step_near):
        return lax.rem(home + 2 * jump, far) * near + lax.rem(my_near + step_near, near)

    loads = []
    for g in range(chunks):
        at = 0
        for k, (ref, cols) in enumerate(((r.w_x, xc), (r.w_z, xc), (r.w_b, bc), (r.w_c, bc))):
            copy = pltpu.make_async_copy(
                ref.at[:, pl.ds(g * cols, cols)], r.wbuf.at[g, :, pl.ds(at, cols)], r.w_sems.at[g, k]
            )
            loads.append(copy)
            at += cols
    rate_load = pltpu.make_async_copy(
        r.w_dt.at[
            pl.ds(pl.multiple_of(column * heads, heads), heads),
            pl.ds(pl.multiple_of(mine * slab, slab), slab),
        ],
        r.wrate,
        r.w_sems.at[chunks, 0],
    )
    out_load = pltpu.make_async_copy(r.w_out, r.w_vm, r.w_sems.at[chunks, 1])
    state_loads = [
        pltpu.make_async_copy(
            r.state.at[:, pl.ds(HPG * g, HPG)], r.state_vm.at[g], r.state_sems.at[g]
        )
        for g in range(chunks)
    ]
    rate_load.start()
    for copy in loads + state_loads + [out_load]:
        copy.start()

    barrier = pltpu.get_barrier_semaphore()

    def greet(target):
        pl.semaphore_signal(barrier, inc=1, device_id=target, device_id_type=MESH)

    count = 0
    for peer in (
        [place(my_far, 0, step) for step in range(1, near)]
        + [place(partner, 0, 0)]
        + [place(my_far, jump, 0) for jump in range(1, half)]
    ):
        greet((peer, column))
        count += 1
    for other in range(1, CORES):
        greet((mine, level * CORES + lax.rem(core + other, CORES)))
        count += 1

    @pl.when(level != owner_level)
    def _():
        greet((mine, owner_level * CORES + core))

    for up in range(1, depth):

        @pl.when(level == owner_level)
        def _():
            greet((mine, lax.rem(level + up, depth) * CORES + core))

    for n in range(ratio):
        for c in range(CORES):
            source = column * ratio + n

            @pl.when(jnp.logical_or(source != mine, c != core))
            def _():
                greet((source, level * CORES + c))

    def barrier_wait():
        @pl.when(level != owner_level)
        def _():
            pl.semaphore_wait(barrier, count + 1)

        @pl.when(jnp.logical_and(level == owner_level, core != owner_core))
        def _():
            pl.semaphore_wait(barrier, count + depth - 1 + ranks)

        @pl.when(jnp.logical_and(level == owner_level, core == owner_core))
        def _():
            pl.semaphore_wait(barrier, count + depth - 1 + ranks - 1)

    copies = []
    waits = {}

    def send(key, source, landing, send_sem, recv_sem, target):
        copy = pltpu.make_async_remote_copy(
            src_ref=source,
            dst_ref=landing,
            send_sem=send_sem,
            recv_sem=recv_sem,
            device_id=(target, column),
            device_id_type=MESH,
        )
        copy.start()
        copies.append(copy)
        waits[key] = copy

    def scale_tokens():
        rate_load.wait()
        gain = r.gain_in[:, pl.ds(pl.multiple_of(mine * slab, slab), slab)]
        rate_w = r.wrate[...]

        @pl.loop(0, ranks)
        def _(d):
            tokens = r.tokens[:, pl.ds(pl.multiple_of(d * seqs, seqs), seqs), :]
            tokens = tokens.astype(F32).reshape(rows, slab)
            block = (tokens * gain).astype(BF16)
            r.scaled[d] = block
            squares = jnp.sum(tokens * tokens, axis=1, keepdims=True)
            r.side_part[d, :, 0:heads] = dot_nt(block, rate_w).astype(BF16)
            r.side_part[d, :, heads : heads + 1] = squares.astype(BF16)

    def multiply(g):
        for copy in loads[4 * g : 4 * g + 4]:
            copy.wait()

        @pl.loop(0, ranks // 2)
        def _(turn):
            block = r.scaled[pl.ds(2 * turn, 2)].reshape(2 * rows, slab)
            both = dot(block, r.wbuf[g]).astype(BF16)
            for k in range(2):
                r.part[g, 2 * turn + k] = both[k * rows : (k + 1) * rows, :first]
                r.zpart[g, 2 * turn + k] = both[k * rows : (k + 1) * rows, first:]

    order = [(jump, kind) for jump in list(range(1, half)) + [0] for kind in range(2)]
    turns = len(order)
    homes = (partner, my_far)
    side = Stream(
        chunks, r.side_part, r.side_near, r.side_made, r.side_pair, r.side_onward, r.side_far
    )
    streams = []
    for g in range(chunks):
        stream = Stream(
            g,
            r.part.at[g],
            r.near_in.at[g],
            r.made.at[g],
            r.pair_in.at[g],
            r.onward.at[g],
            r.far_in.at[g],
        )
        streams.append([side, stream] if g == 0 else [stream])

    def start_near(q):
        g, t = q // turns, q % turns
        jump, kind = order[t]
        slot = 2 * jump + kind
        for step in range(1, near):
            for s in streams[g]:
                send(
                    ("near", s.index, slot, step),
                    s.part.at[place(homes[kind], jump, step)],
                    s.near.at[slot, step - 1],
                    r.near_s.at[s.index, slot, step - 1],
                    r.near_r.at[s.index, slot, step - 1],
                    place(my_far, 0, step),
                )

    def start_zpair(g):
        for jump in list(range(1, half)) + [0]:
            for step in range(near):
                send(
                    ("zpair", g, jump, step),
                    r.zpart.at[g, place(partner, jump, step)],
                    r.zpair.at[g, jump, step],
                    r.zpair_s.at[g, jump, step],
                    r.zpair_r.at[g, jump, step],
                    place(partner, 0, 0),
                )

    def near_terms(s, slot):
        return [s.near[slot, step - 1] for step in range(1, near)]

    def reduce_step(g, t):
        jump, kind = order[t]
        slot = 2 * jump + kind
        for s in streams[g]:
            for step in range(1, near):
                waits["near", s.index, slot, step].wait_recv()
            if kind == 0:
                s.made[jump] = sum_of(
                    s.part[place(partner, jump, 0)], near_terms(s, slot)
                ).astype(BF16)
                send(
                    ("pair", s.index, jump),
                    s.made.at[jump],
                    s.pair.at[jump],
                    r.pair_s.at[s.index, jump],
                    r.pair_r.at[s.index, jump],
                    place(partner, 0, 0),
                )
            elif jump > 0:
                waits["pair", s.index, jump].wait_recv()
                s.onward[jump - 1] = sum_of(
                    s.part[place(my_far, jump, 0)], near_terms(s, slot) + [s.pair[jump]]
                ).astype(BF16)
                send(
                    ("far", s.index, jump),
                    s.onward.at[jump - 1],
                    s.landed.at[jump - 1],
                    r.far_s.at[s.index, jump - 1],
                    r.far_r.at[s.index, jump - 1],
                    place(my_far, jump, 0),
                )

    def z_onward(g):
        for jump in range(1, half):
            for step in range(near):
                waits["zpair", g, jump, step].wait_recv()
                r.zonward[g, jump - 1, step] = sum_of(
                    r.zpart[g, place(my_far, jump, step)], [r.zpair[g, jump, step]]
                ).astype(BF16)
                send(
                    ("zfar", g, jump, step),
                    r.zonward.at[g, jump - 1, step],
                    r.zfar.at[g, jump - 1, step],
                    r.zfar_s.at[g, jump - 1, step],
                    r.zfar_r.at[g, jump - 1, step],
                    place(my_far, jump, 0),
                )

    def z_terms(g, step):
        return [r.zpair[g, 0, step]] + [r.zfar[g, jump - 1, step] for jump in range(1, half)]

    def z_last(g):
        for step in range(near):
            waits["zpair", g, 0, step].wait_recv()
            for jump in range(1, half):
                waits["zfar", g, jump, step].wait_recv()
        for step in range(1, near):
            r.zfin_out[g, step - 1] = sum_of(
                r.zpart[g, place(my_far, 0, step)], z_terms(g, step)
            ).astype(BF16)
            send(
                ("zfin", g, step),
                r.zfin_out.at[g, step - 1],
                r.zfin_in.at[g, step - 1],
                r.zfin_s.at[g, step - 1],
                r.zfin_r.at[g, step - 1],
                place(my_far, 0, step),
            )

    def finish(g):
        for s in streams[g]:
            waits["pair", s.index, 0].wait_recv()
            for jump in range(1, half):
                waits["far", s.index, jump].wait_recv()
            total = sum_of(
                s.part[mine],
                near_terms(s, 1) + [s.pair[0]] + [s.landed[jump - 1] for jump in range(1, half)],
            )
            if s is side:
                scale = lax.rsqrt(total[:, heads : heads + 1] / width + EPS)
                r.scale[...] = scale
                rates(total[:, 0:heads] * scale)
            else:
                total = (total * r.scale[...]).astype(BF16)
                r.here[g, :, 0:xc] = total[:, :xc]
                r.gate[g] = total[:, xc : 2 * xc]
                r.here[g, :, xc : xc + bc] = total[:, 2 * xc :]
        for step in range(1, near):
            waits["zfin", g, step].wait_recv()
        total = sum_of(
            r.zpart[g, mine], z_terms(g, 0) + [r.zfin_in[g, step - 1] for step in range(1, near)]
        )
        r.here[g, :, xc + bc :] = (total * r.scale[...]).astype(BF16)

    bias = r.bias[...]
    a_rate = -jnp.exp(r.a_log[...])

    def tap(k, g, parts):
        held = ((r.conv_wx, xc), (r.conv_wb, bc), (r.conv_wc, bc))
        return jnp.concatenate(
            [ref[k : k + 1, g * cols : (g + 1) * cols].astype(F32) for ref, cols in held[:parts]],
            axis=1,
        )

    def accepted_column():
        eye = iota((seqs, seqs), 0) == iota((seqs, seqs), 1)
        return jnp.sum(jnp.where(eye, r.accepted[...].astype(F32), 0.0), axis=1, keepdims=True)

    def replay_weights():
        accepted = jnp.concatenate([accepted_column()] * path_len, axis=0)
        step_of = lax.shift_right_logical(iota((prows, 1), 0), shift).astype(F32)
        live = (step_of < accepted).astype(F32)
        path_step = softplus(r.path_dt[...].astype(F32).reshape(prows, heads) + bias)
        log_decay = path_step * a_rate * live
        pr, pc = iota((prows, prows), 0), iota((prows, prows), 1)
        later = jnp.where(((pr & low) == (pc & low)) & (pc > pr), 1.0, 0.0)
        every = jnp.where(iota((seqs, prows), 0) == (iota((seqs, prows), 1) & low), 1.0, 0.0)
        r.weights[...] = live * jnp.exp(dot_high(later, log_decay)) * path_step
        r.overall[...] = jnp.exp(dot_high(every, log_decay))

    def replay(g):
        at = 0
        for conv, path, cols in (
            (r.conv_x, r.path_x, xc),
            (r.conv_b, r.path_b, bc),
            (r.conv_c, r.path_c, bc),
        ):
            span = slice(g * cols, (g + 1) * cols)
            top = conv[:, :, span].astype(F32).reshape(keep * seqs, cols)
            end = path[:, :, span].astype(F32).reshape(prows, cols)
            r.hist[:, at : at + cols] = jnp.concatenate([top, end], axis=0).astype(BF16)
            at += cols
        values = r.hist[:, 0 : xc + bc].astype(F32)
        summed = tap(0, g, 2) * values[0:prows]
        for k in range(1, taps):
            summed = summed + tap(k, g, 2) * values[k * seqs : k * seqs + prows]
        post = silu(summed)
        left = (post[:, :xc] * spread(r.weights[...], g, xc)).T.astype(BF16)
        block_mask = (iota((prows, seqs * bc), 0) & low) == lax.shift_right_logical(
            iota((prows, seqs * bc), 1), bc_shift
        )
        right = jnp.where(block_mask, jnp.concatenate([post[:, xc:]] * seqs, axis=1), 0.0)
        grown = dot(left, right.astype(BF16))
        overall = r.overall[...]
        state_loads[g].wait()
        for s in range(seqs):
            for i in range(HPG):
                h = HPG * g + i
                fresh = (
                    overall[s : s + 1, h : h + 1] * r.state_vm[g, s, i]
                    + grown[i * head_dim : (i + 1) * head_dim, s * bc : (s + 1) * bc]
                )
                r.state_vm[g, s, i] = fresh
                r.new_bf[
                    g, i * head_dim : (i + 1) * head_dim, s * bc : (s + 1) * bc
                ] = fresh.astype(BF16)
        new_copy(g).start()
        reached = dot(r.all_h[...], r.hist[...])
        summed = tap(taps - 2, g, 3) * reached[0:rows]
        for k in range(2, taps):
            summed = summed + tap(taps - 1 - k, g, 3) * reached[(k - 1) * rows : k * rows]
        r.before[g] = summed

    def new_copy(g):
        return pltpu.make_async_copy(
            r.state_vm.at[g], r.new_state.at[:, pl.ds(HPG * g, HPG)], r.new_sems.at[g]
        )

    def tree():
        parents = r.parents[...].astype(F32)
        parent = jnp.concatenate([parents[:, i : i + 1] for i in range(props)], axis=0)
        accepted = jnp.concatenate([accepted_column()] * props, axis=0)
        seq_of = (iota((rows, 1), 0) & low).astype(F32)
        in_tree = parent >= 0.0
        hist_at = jnp.where(in_tree, -1.0, (accepted + (keep - 1)) * seqs + seq_of)
        prop_at = jnp.where(in_tree, parent * seqs + seq_of, -1.0)
        link_p = iota((rows, rows), 1).astype(F32) == prop_at
        link_h = iota((rows, hrows), 1).astype(F32) == hist_at
        up_p = jnp.where(link_p, 1.0, 0.0).astype(BF16)
        up_h = jnp.where(link_h, 1.0, 0.0).astype(BF16)
        back = jnp.where(
            iota((hrows, hrows), 1) == iota((hrows, hrows), 0) - seqs, 1.0, 0.0
        ).astype(BF16)
        last_p, last_h = up_p, up_h
        r.all_p[0:rows] = last_p
        r.all_h[0:rows] = last_h
        for k in range(1, taps - 1):
            last_p, last_h = (
                dot(last_p, up_p).astype(BF16),
                (dot(last_p, up_h) + dot(last_h, back)).astype(BF16),
            )
            r.all_p[k * rows : (k + 1) * rows] = last_p
            r.all_h[k * rows : (k + 1) * rows] = last_h
        self_at = iota((rows, rows), 0) == iota((rows, rows), 1)
        above = jnp.where(link_p | self_at, 1.0, 0.0)
        for _ in range((props - 1).bit_length()):
            some = above.astype(BF16)
            above = jnp.minimum(dot(some, some), 1.0)
        r.above[...] = above

    def rates(rate_rows):
        step_size = softplus(rate_rows.astype(BF16).astype(F32) + bias)
        decay = dot_high(r.above[...], step_size * a_rate)
        r.decay[...] = decay
        r.decay_t[...] = decay.T
        r.step_t[...] = step_size.T

    def mix(g):
        here = r.here[g]
        summed = r.before[g] + tap(taps - 1, g, 3) * here.astype(F32)
        reached = dot(r.all_p[...], here)
        for k in range(1, taps):
            summed = summed + tap(taps - 1 - k, g, 3) * reached[(k - 1) * rows : k * rows]
        post = silu(summed)
        post_x = post[:, :xc]
        post_b = post[:, xc : xc + bc].astype(BF16)
        post_c = post[:, xc + bc :]
        scores = dot_nt(post_c.astype(BF16), post_b)
        decay = r.decay[...]
        above = r.above[...] > 0.5
        lane = iota((1, xc), 1)
        own = (iota((rows, seqs * bc), 0) & low) == lax.shift_right_logical(
            iota((rows, seqs * bc), 1), bc_shift
        )
        wide_c = jnp.where(own, jnp.concatenate([post_c] * seqs, axis=1), 0.0).astype(BF16)
        carried = dot_nt(wide_c, r.new_bf[g])
        out = carried * spread(jnp.exp(decay), g, xc) + spread(r.skip[...], g, xc) * post_x
        for i in range(HPG):
            h = HPG * g + i
            gap = decay[:, h : h + 1] - r.decay_t[h : h + 1, :]
            mixing = jnp.where(above, jnp.exp(jnp.where(above, gap, 0.0)), 0.0)
            mixing = scores * mixing * r.step_t[h : h + 1, :]
            head = (lane >= i * head_dim) & (lane < (i + 1) * head_dim)
            out = out + dot(mixing.astype(BF16), jnp.where(head, post_x, 0.0).astype(BF16))
        out = out * silu(r.gate[g].astype(F32))
        out = out * lax.rsqrt(jnp.mean(out * out, axis=1, keepdims=True) + EPS)
        r.gathered[g, 0] = (out * r.gain_out[:, g * xc : (g + 1) * xc]).astype(BF16)

    index = {}
    for home in range(2):
        for jump in range(half):
            for step in range(near):
                index[jump, home, step] = len(index)
    sources = (my_far, partner)

    def origin(key):
        jump, home, step = key
        return lax.rem(sources[home] + far - 2 * jump, far) * near + lax.rem(
            my_near + near - step, near
        )

    def gather(g, source, key, target):
        k = index[key]
        send(
            ("gather", g, key),
            r.gathered.at[g, index[source]],
            r.gathered.at[g, k],
            r.gather_s.at[g, k],
            r.gather_r.at[g, k],
            target,
        )

    def gather_own(g):
        for jump in range(1, half):
            gather(g, (0, 0, 0), (jump, 0, 0), place(my_far, jump, 0))
        gather(g, (0, 0, 0), (0, 1, 0), place(partner, 0, 0))
        for step in range(1, near):
            gather(g, (0, 0, 0), (0, 0, step), place(my_far, 0, step))

    def gather_on(g, home, jumps):
        for jump in jumps:
            key = (jump, home, 0)
            waits["gather", g, key].wait_recv()
            if home == 0:
                gather(g, key, (jump, 1, 0), place(partner, 0, 0))
            for step in range(1, near):
                gather(g, key, (jump, home, step), place(my_far, 0, step))

    jumps = list(range(1, half))

    def gather_1(g):
        gather_on(g, 0, jumps)

    def gather_2(g):
        gather_on(g, 1, [0])

    def gather_3(g):
        gather_on(g, 1, jumps)

    def add_terms(g, keys):
        weight = r.w_vm[g * xc : (g + 1) * xc, :]
        for key in keys:
            k = index[key]
            term = dot(r.gathered[g, k], weight)
            if g > 0:
                term = r.sums[k] + term
            if g < chunks - 1:
                r.sums[k] = term
            else:
                r.terms[k] = term.astype(BF16)

    def gather_end(g):
        for home in range(2):
            for jump in range(half):
                for step in range(1, near):
                    waits["gather", g, (jump, home, step)].wait_recv()
        add_terms(g, list(index))

    arrival = [(0, 0, 0)] + [(jump, 0, 0) for jump in jumps]
    arrival += [(0, 1, 0)] + [(0, 0, step) for step in range(1, near)]
    arrival += [(jump, 1, 0) for jump in jumps]
    arrival += [(jump, 0, step) for jump in jumps for step in range(1, near)]
    arrival += [(jump, 1, step) for jump in range(half) for step in range(1, near)]
    batches = [arrival[at : at + CORES] for at in range(0, len(arrival), CORES)]

    def pick(options, which):
        out = options[0]
        for k in range(1, CORES):
            out = jnp.where(which == k, options[k], out)
        return out

    def slots(n):
        return [index[key] for key in batches[n]]

    def sibling_copy(n, other):
        target = lax.rem(core + other, CORES)
        return pltpu.make_async_remote_copy(
            src_ref=r.terms.at[pick(slots(n), target)],
            dst_ref=r.sibling_in.at[n, other - 1],
            send_sem=r.sib_s.at[n, other - 1],
            recv_sem=r.sib_r.at[n, other - 1],
            device_id=(mine, level * CORES + target),
            device_id_type=MESH,
        )

    def column_copy(n, up):
        return pltpu.make_async_remote_copy(
            src_ref=r.paired.at[n],
            dst_ref=r.column_in.at[n, up - 1],
            send_sem=r.col_s.at[n],
            recv_sem=r.col_r.at[n, up - 1],
            device_id=(mine, owner_level * CORES + core),
            device_id_type=MESH,
        )

    def done_copy(n):
        return pltpu.make_async_remote_copy(
            src_ref=r.done.at[n],
            dst_ref=r.arrived.at[spot],
            send_sem=r.done_s.at[n],
            recv_sem=r.done_r.at[spot],
            device_id=(pick([origin(key) for key in batches[n]], core), owner),
            device_id_type=MESH,
        )

    def stays(n):
        if (0, 0, 0) not in batches[n]:
            return None
        return jnp.logical_and(core == batches[n].index((0, 0, 0)), owner == column)

    def pair_up(n):
        total = r.terms[pick(slots(n), core)].astype(F32)
        for other in range(1, CORES):
            sibling_copy(n, other).wait_recv()
            total = total + r.sibling_in[n, other - 1].astype(F32)
        r.paired[n] = total.astype(BF16)
        for up in range(1, depth):

            @pl.when(lax.rem(level - owner_level + depth, depth) == up)
            def _():
                column_copy(n, up).start()

    def send_done(n):
        @pl.when(level == owner_level)
        def _():
            total = r.paired[n].astype(F32)
            for up in range(1, depth):
                column_copy(n, up).wait_recv()
                total = total + r.column_in[n, up - 1].astype(F32)
            r.done[n] = total.astype(BF16)
            here = stays(n)
            if here is None:
                done_copy(n).start()
            else:

                @pl.when(here)
                def _():
                    r.arrived[spot] = r.done[n]

                @pl.when(jnp.logical_not(here))
                def _():
                    done_copy(n).start()

    total_turns = chunks * turns
    ahead = min(AHEAD, total_turns)
    multiplied = [0]

    def near_turn(q):
        if q < total_turns:
            if q // turns > multiplied[0]:
                multiplied[0] += 1
                multiply(multiplied[0])
            start_near(q)

    scale_tokens()
    multiply(0)
    barrier_wait()
    for q in range(ahead):
        near_turn(q)
    start_zpair(0)
    tree()
    replay_weights()
    out_load.wait()
    fillers = [functools.partial(replay, g) for g in range(chunks)]
    last = chunks - 1
    for g in range(chunks):
        for t in range(turns):
            reduce_step(g, t)
            near_turn(g * turns + t + ahead)
            if t == 0:
                z_onward(g)
                if g >= 2:
                    gather_3(g - 2)
            if t == 1 and g < last:
                if g + 1 > multiplied[0]:
                    multiplied[0] += 1
                    multiply(multiplied[0])
                start_zpair(g + 1)
            if t == turns - 2:
                z_last(g)
            if g == 0 and len(fillers) > 0:
                fillers.pop(0)()
            if t == 0 and g >= 1:
                while len(fillers) > 0:
                    fillers.pop(0)()
                finish(g - 1)
                mix(g - 1)
                gather_own(g - 1)
            if t == 1 and g >= 2:
                gather_end(g - 2)
            if t == turns - 2 and g >= 1:
                gather_1(g - 1)
            if t == turns - 1 and g >= 1:
                gather_2(g - 1)
    while len(fillers) > 0:
        fillers.pop(0)()
    if last >= 1:
        gather_3(last - 1)
    finish(last)
    mix(last)
    gather_own(last)
    if last >= 1:
        gather_end(last - 1)

    for n, keys in enumerate(batches):
        for key in keys:
            if key != (0, 0, 0):
                jump, home, step = key
                if step == 0:
                    gather_on(last, home, [jump])
                else:
                    waits["gather", last, key].wait_recv()
            add_terms(last, [key])
        for other in range(1, CORES):
            sibling_copy(n, other).start()
        if n >= 1:
            pair_up(n - 1)
        if n >= 2:
            send_done(n - 2)
    final = len(batches) - 1
    pair_up(final)
    if final >= 1:
        send_done(final - 1)
    send_done(final)

    for n in range(ratio):
        source = column * ratio + n
        local = jnp.logical_and(source == mine, core == batches[0].index((0, 0, 0)))

        @pl.when(jnp.logical_not(local))
        def _():
            pltpu.make_async_remote_copy(
                src_ref=r.done.at[0],
                dst_ref=r.arrived.at[n],
                send_sem=r.done_s.at[0],
                recv_sem=r.done_r.at[n],
                device_id=(source, lax.rem(column + 1, blocks)),
                device_id_type=MESH,
            ).wait_recv()

        r.mixed[:, n * out_slab : (n + 1) * out_slab] = r.arrived[n]

    for g in range(chunks):
        new_copy(g).wait()
    for copy in copies:
        copy.wait_send()
    for n in range(len(batches)):
        for other in range(1, CORES):
            sibling_copy(n, other).wait_send()

        @pl.when(level != owner_level)
        def _():
            column_copy(n, 1).wait_send()

        @pl.when(level == owner_level)
        def _():
            here = stays(n)
            if here is None:
                done_copy(n).wait_send()
            else:

                @pl.when(jnp.logical_not(here))
                def _():
                    done_copy(n).wait_send()


def run_mixer(inputs, ranks, blocks):
    tokens, w_x, state = inputs["tokens"], inputs["w_x"], inputs["state"]
    props, all_seqs, slab = tokens.shape
    seqs, heads, head_dim, state_dim = state.shape
    rows = props * seqs
    near = inner_size(ranks)
    far = ranks // near
    half = far // 2
    chunks = heads // HPG
    ratio = ranks // blocks
    depth = blocks // CORES
    batches = ranks // CORES
    xc, bc = HPG * head_dim, state_dim
    wide = 2 * xc + bc
    out_slab = inputs["w_out"].shape[1]
    keep = inputs["conv_x"].shape[0]
    held = (keep + inputs["path_x"].shape[0]) * seqs
    prows = inputs["path_x"].shape[0] * seqs
    vmem = pl.BlockSpec(memory_space=pltpu.VMEM)
    hbm = pl.BlockSpec(memory_space=pl.ANY)
    dma = pltpu.SemaphoreType.DMA

    def buf(*shape):
        return pltpu.VMEM(shape, BF16)

    def full(*shape):
        return pltpu.VMEM(shape, F32)

    scratch = dict(
        wbuf=buf(chunks, slab, wide + bc),
        wrate=buf(heads, slab),
        w_vm=buf(w_x.shape[1], out_slab),
        scaled=buf(ranks, rows, slab),
        part=buf(chunks, ranks, rows, wide),
        near_in=buf(chunks, far, near - 1, rows, wide),
        made=buf(chunks, half, rows, wide),
        pair_in=buf(chunks, half, rows, wide),
        onward=buf(chunks, half - 1, rows, wide),
        far_in=buf(chunks, half - 1, rows, wide),
        side_part=buf(ranks, rows, LANES),
        side_near=buf(far, near - 1, rows, LANES),
        side_made=buf(half, rows, LANES),
        side_pair=buf(half, rows, LANES),
        side_onward=buf(half - 1, rows, LANES),
        side_far=buf(half - 1, rows, LANES),
        zpart=buf(chunks, ranks, rows, bc),
        zpair=buf(chunks, half, near, rows, bc),
        zonward=buf(chunks, half - 1, near, rows, bc),
        zfar=buf(chunks, half - 1, near, rows, bc),
        zfin_out=buf(chunks, near - 1, rows, bc),
        zfin_in=buf(chunks, near - 1, rows, bc),
        scale=full(rows, 1),
        here=buf(chunks, rows, xc + 2 * bc),
        gate=buf(chunks, rows, xc),
        state_vm=full(chunks, seqs, HPG, head_dim, state_dim),
        new_bf=buf(chunks, xc, seqs * bc),
        weights=full(prows, heads),
        overall=full(seqs, heads),
        hist=buf(held, xc + 2 * bc),
        before=full(chunks, rows, xc + 2 * bc),
        all_p=buf(keep * rows, rows),
        all_h=buf(keep * rows, held),
        above=full(rows, rows),
        decay=full(rows, heads),
        decay_t=full(heads, rows),
        step_t=full(heads, rows),
        gathered=buf(chunks, ranks, rows, xc),
        sums=full(ranks, rows, out_slab),
        terms=buf(ranks, rows, out_slab),
        sibling_in=buf(batches, CORES - 1, rows, out_slab),
        paired=buf(batches, rows, out_slab),
        column_in=buf(batches, depth - 1, rows, out_slab),
        done=buf(batches, rows, out_slab),
        arrived=buf(ratio, rows, out_slab),
        w_sems=dma((chunks + 1, 4)),
        state_sems=dma((chunks,)),
        new_sems=dma((chunks,)),
        near_s=dma((chunks + 1, far, near - 1)),
        near_r=dma((chunks + 1, far, near - 1)),
        pair_s=dma((chunks + 1, half)),
        pair_r=dma((chunks + 1, half)),
        far_s=dma((chunks + 1, half - 1)),
        far_r=dma((chunks + 1, half - 1)),
        zpair_s=dma((chunks, half, near)),
        zpair_r=dma((chunks, half, near)),
        zfar_s=dma((chunks, half - 1, near)),
        zfar_r=dma((chunks, half - 1, near)),
        zfin_s=dma((chunks, near - 1)),
        zfin_r=dma((chunks, near - 1)),
        gather_s=dma((chunks, ranks)),
        gather_r=dma((chunks, ranks)),
        sib_s=dma((batches, CORES - 1)),
        sib_r=dma((batches, CORES - 1)),
        col_s=dma((batches,)),
        col_r=dma((batches, depth - 1)),
        done_s=dma((batches,)),
        done_r=dma((ratio,)),
    )
    in_hbm = ("w_x", "w_z", "w_b", "w_c", "w_dt", "w_out", "state")
    names = tuple(inputs) + ("mixed", "new_state") + tuple(scratch)
    return pl.pallas_call(
        functools.partial(mixer_kernel, names, near, far, chunks, ratio),
        out_shape=(
            jax.ShapeDtypeStruct((rows, ratio * out_slab), BF16),
            jax.ShapeDtypeStruct(state.shape, F32),
        ),
        in_specs=[hbm if name in in_hbm else vmem for name in inputs],
        out_specs=(vmem, hbm),
        scratch_shapes=list(scratch.values()),
        compiler_params=pltpu.CompilerParams(collective_id=0, has_side_effects=True),
        name="mixer",
    )(*inputs.values())


def store_kernel(pieces, mixed_in, state_in, mixed_out, state_out, held, ins, outs, last):
    step = held.shape[1]
    reads, writes = [], []
    for k in range(pieces):
        reads.append(
            pltpu.make_async_copy(state_in.at[pl.ds(k * step, step)], held.at[k], ins.at[k])
        )
        writes.append(
            pltpu.make_async_copy(held.at[k], state_out.at[pl.ds(k * step, step)], outs.at[k])
        )
        reads[k].start()
    copy = pltpu.make_async_copy(mixed_in, mixed_out, last)
    copy.start()
    for k in range(pieces):
        reads[k].wait()
        writes[k].start()
    for k in range(pieces):
        writes[k].wait()
    copy.wait()


def store(mixed, state):
    pieces = state.shape[0]
    vmem = pl.BlockSpec(memory_space=pltpu.VMEM)
    hbm = pl.BlockSpec(memory_space=pl.ANY)
    dma = pltpu.SemaphoreType.DMA
    return pl.pallas_call(
        functools.partial(store_kernel, pieces),
        out_shape=(
            jax.ShapeDtypeStruct(mixed.shape, mixed.dtype),
            jax.ShapeDtypeStruct(state.shape, state.dtype),
        ),
        in_specs=[vmem, hbm],
        out_specs=(hbm, hbm),
        scratch_shapes=[
            pltpu.VMEM((pieces, state.shape[0] // pieces) + state.shape[1:], F32),
            dma((pieces,)),
            dma((pieces,)),
            dma(()),
        ],
        name="store",
    )(mixed, state)


def shards(
    tokens,
    parents,
    accepted,
    state,
    conv_x,
    conv_b,
    conv_c,
    path_x,
    path_b,
    path_c,
    path_dt,
    gain_in,
    w_x,
    w_z,
    w_b,
    w_c,
    w_dt,
    dt_bias,
    a_log,
    d_skip,
    conv_wx,
    conv_wb,
    conv_wc,
    gain_out,
    w_out,
):
    ranks = lax.axis_size("kv")
    blocks = lax.axis_size("tp")

    def front(array):
        return jnp.swapaxes(array, 0, 1)

    summed, new_state = run_mixer(
        dict(
            tokens=front(tokens),
            parents=parents,
            accepted=accepted[None, :],
            state=state,
            conv_x=front(conv_x),
            conv_b=front(conv_b),
            conv_c=front(conv_c),
            path_x=front(path_x),
            path_b=front(path_b),
            path_c=front(path_c),
            path_dt=front(path_dt),
            gain_in=gain_in[None, :],
            w_x=w_x,
            w_z=w_z,
            w_b=w_b,
            w_c=w_c,
            w_dt=w_dt.T,
            bias=dt_bias[None, :],
            a_log=a_log[None, :],
            skip=d_skip[None, :],
            conv_wx=conv_wx,
            conv_wb=conv_wb,
            conv_wc=conv_wc,
            gain_out=gain_out[None, :],
            w_out=w_out,
        ),
        ranks,
        blocks,
    )
    summed, new_state = store(summed, new_state)
    seqs, props = parents.shape
    mixed = front(summed.reshape(props, seqs, summed.shape[1]))
    return (mixed, new_state)


def solution(mesh):
    return jax.shard_map(
        shards,
        mesh=mesh,
        in_specs=(
            P(None, None, "kv"),
            P("kv", None),
            P("kv"),
            P("kv", "tp", None, None),
            P("kv", None, "tp"),
            P("kv", None, "tp"),
            P("kv", None, "tp"),
            P("kv", None, "tp"),
            P("kv", None, "tp"),
            P("kv", None, "tp"),
            P("kv", None, "tp"),
            P(),
            P("kv", "tp"),
            P("kv", "tp"),
            P("kv", "tp"),
            P("kv", "tp"),
            P(),
            P("tp"),
            P("tp"),
            P("tp"),
            P(None, "tp"),
            P(None, "tp"),
            P(None, "tp"),
            P("tp"),
            P("tp", "kv"),
        ),
        out_specs=(P("kv", None, "tp"), P("kv", "tp", None, None)),
        check_vma=False,
    )
```
